32 devices in a mesh: sp: 8 (over z, x), tp: 4 (over y, core).
Axes of the slice: x: 2, y: 2, z: 4, core: 2. Of those that a mesh axis runs over, the one named last changes fastest.
Arguments:
- out_grad: bfloat16 [1024, 2048], P('sp', 'tp'), may hold values from -6 to 6
- moe_input: bfloat16 [1024, 2048], P('sp', 'tp'), may hold values from -6 to 6
- route_weight: float32 [1024, 2], P('sp'), may hold values from 0.2 to 1
- route_ids: int32 [1024, 2], P('sp'), may hold values from 0 to 7, all different within a row; in each aligned block of 128 rows (0 to 127, 128 to 255, ...) at most 64 rows name the same one
- gate_proj: bfloat16 [8, 2048, 2816], P('sp', None, 'tp'), may hold values from -0.125 to 0.125
- up_proj: bfloat16 [8, 2048, 2816], P('sp', None, 'tp'), may hold values from -0.125 to 0.125
- down_proj: bfloat16 [8, 2816, 2048], P('sp', 'tp'), may hold values from -0.109375 to 0.109375
- out_proj: bfloat16 [2048, 2048], P(None, 'tp'), may hold values from -0.125 to 0.125
- conv_out: bfloat16 [1024, 2048], P('sp', 'tp'), may hold values from -6 to 6
- gate_b: bfloat16 [1024, 2048], P('sp', 'tp'), may hold values from -6 to 6
- gate_c: bfloat16 [1024, 2048], P('sp', 'tp'), may hold values from -6 to 6
- value_v: bfloat16 [1024, 2048], P('sp', 'tp'), may hold values from -6 to 6
- conv_taps: float32 [3, 2048], P(None, 'tp'), may hold values from -3 to 3
Outputs:
- grad_gate: bfloat16 [8, 2048, 2816], P('sp', None, 'tp')
- grad_up: bfloat16 [8, 2048, 2816], P('sp', None, 'tp')
- grad_down: bfloat16 [8, 2816, 2048], P('sp', 'tp')
- grad_out: float32 [2048, 2048], P('sp', 'tp')
- grad_b: bfloat16 [1024, 2048], P('sp', 'tp')
- grad_c: bfloat16 [1024, 2048], P('sp', 'tp')
- grad_v: bfloat16 [1024, 2048], P('sp', 'tp')
The draws below stay inside these ranges and needn't reach their ends.
Inputs may be any that keep to these rules, and one draw needn't show every extreme that they name: `route_ids`: each row names two different experts; within the 128 rows of one index of sp no expert is named by more than 64 rows, a bound that some block reaches.
All inputs are finite; a program needn't handle non-finite values.
Results may differ from the reference program's by a relative error of at most 0.019.
Values may be sent and summed in bfloat16 or wider, within the bound.
A program may use at most 64 MiB of HBM per device.

```python
import math
import jax
import jax.numpy as jnp
import numpy as np
from jax import lax

D = 2048
FF = 2816
TOK_DEV = 128
TOKENS = 1024
EXPERTS = 8
CAP = 64
N_SP = 8
N_TP = 4


def with_spikes(drawn, key, source, target, shards_of, factor):
    owner, partner = [(jnp.arange(drawn.shape[axis_at]) // (drawn.shape[axis_at] // shards_of)).reshape([-1 if axis == axis_at else 1 for axis in range(drawn.ndim)]) for axis_at in (source, target)]
    chosen = jax.random.permutation(key, shards_of)[partner]
    strong = (owner == chosen) | (owner == (partner + shards_of // 2) % shards_of)
    return jnp.where(strong, factor * drawn, drawn)


def block_levels(rng, shape, pieces, smallest, top_value):
    def one(axis_at, blocks):
        heights = jax.random.uniform(jax.random.fold_in(jax.random.fold_in(rng, 6), axis_at), (blocks,), jnp.float32, smallest / len(pieces), top_value / len(pieces))
        return jnp.repeat(jnp.exp(heights), shape[axis_at] // blocks).reshape((-1,) + (1,) * (len(shape) - axis_at - 1))

    level = one(*pieces[0])
    for cut in pieces[1:]:
        level = level * one(*cut)
    return level


def routed_block(key, own, number, rows, amount, top, bound, skew):
    order = jax.random.permutation(key, amount)
    crowded, ordinary = portions_of(amount, rows * top, bound, skew, True), portions_of(amount, rows * top, bound, skew, False)
    places = jnp.arange(amount)

    def named(sizes, rotation):
        used = int((sizes > 0).sum())
        fixed = max(1, used // 4)
        passed = fixed + (places - fixed + rotation * (used - fixed)) % max(1, amount - fixed)
        return jnp.zeros((amount,), jnp.int32).at[order[jnp.where(places < fixed, places, passed)]].set(jnp.asarray(sizes, jnp.int32))

    sizes = jnp.where(number % 4 == 0, named(crowded, number // 4), named(ordinary, number - number // 4 - 1))
    mixed = jax.random.permutation(jax.random.fold_in(own, 3), amount)
    donor, sink = mixed[0:amount // 2 * 2:2], mixed[1:amount // 2 * 2:2]
    room = jnp.minimum(sizes[donor] - 1, bound - sizes[sink]) // 2
    room = jnp.where((donor == order[0]) | (sink == order[0]) | (sizes[sink] == 0), 0, jnp.maximum(room, 0))
    passed = jax.random.randint(jax.random.fold_in(own, 4), (amount // 2,), 0, 1 << 20) % (room + 1)
    sizes = sizes.at[donor].add(-passed).at[sink].add(passed)
    labels = jnp.searchsorted(jnp.cumsum(sizes), jnp.arange(rows * top), side="right").astype(jnp.int32)
    grid = labels.reshape(top, rows).T
    grid = grid[jax.random.permutation(jax.random.fold_in(own, 1), rows)]
    rotation = jax.random.randint(jax.random.fold_in(own, 2), (rows, 1), 0, top)
    return jnp.take_along_axis(grid, (jnp.arange(top)[None, :] + rotation) % top, axis=1)


def portions_of(count, total, most, skew, full):
    weights = [(1 << 20) // math.isqrt(standing ** skew) + 1 for standing in range(1, count + 1)]
    largest = most if full else min(most, max(-(-total // count), total * weights[0] // sum(weights)))
    least = 1 if total - largest >= count - 1 else 0
    given, surplus = [largest] + [least] * (count - 1), total - largest - least * (count - 1)
    while surplus > 0:
        movable = [i for i in range(1, count) if given[i] < largest] or [i for i in range(1, count) if given[i] < most]
        mass, left = sum([weights[i] for i in movable]), surplus
        for i in movable:
            addition = min(most - given[i], max(1, left * weights[i] // mass), surplus)
            given[i] = given[i] + addition
            surplus = surplus - addition
    return np.array(given)


def normal_values(rng, shape, deviation, reach, split=(), kind=jnp.bfloat16):
    loudness = block_levels(rng, shape, split, -0.22, 0.18) if split else 1.0
    values = jax.random.normal(rng, shape, jnp.float32) * deviation * loudness
    return jnp.minimum(jnp.maximum(values, -reach), reach).astype(kind)


def bell_draw_with(rng, extent, spread, limit, pieces, heavy, held_as=jnp.bfloat16):
    array = spread * jax.random.normal(rng, extent, jnp.float32)
    if pieces:
        array = array * block_levels(rng, extent, pieces, -0.22, 0.18)
    return jnp.clip(with_spikes(array, jax.random.fold_in(rng, 3), *heavy), -limit, limit).astype(held_as)


def setup_inputs(seed: int = 0) -> dict:
    arg_keys = jax.random.split(jax.random.key(seed), 14)
    out_grad = bell_draw_with(arg_keys[0], (TOKENS, D), 1.0, 6.0, ((0, 8), (1, 4)), (0, 1, 8, 2.0))
    moe_input = normal_values(arg_keys[1], (TOKENS, D), 1.0, 6.0, ((0, 8), (1, 4)))
    route_weight = jnp.clip(jnp.exp(math.log(1.0) - 1.609438 * jax.random.uniform(arg_keys[2], (TOKENS, 2), jnp.float32) ** block_levels(arg_keys[2], (TOKENS, 2), ((0, 8),), -0.2, 0.2)), 0.2, 1.0)
    route_ids_keys = jax.random.split(jax.random.fold_in(arg_keys[3], 1), TOKENS // TOK_DEV)
    route_ids_turns = jax.random.permutation(jax.random.fold_in(arg_keys[3], 3), TOKENS // TOK_DEV)
    route_ids = jax.vmap(lambda own, number: routed_block(jax.random.fold_in(arg_keys[3], 2), own, number, TOK_DEV, EXPERTS, 2, CAP, 1))(route_ids_keys, route_ids_turns).reshape((TOKENS, 2))
    gate_proj = normal_values(arg_keys[4], (EXPERTS, D, FF), D ** -0.5, 0.125, ((0, 8), (2, 4)))
    up_proj = normal_values(arg_keys[5], (EXPERTS, D, FF), D ** -0.5, 0.125, ((0, 8), (2, 4)))
    down_proj = normal_values(arg_keys[6], (EXPERTS, FF, D), FF ** -0.5, 0.109375, ((0, 8), (1, 4)))
    out_proj = normal_values(arg_keys[7], (D, D), D ** -0.5, 0.125, ((1, 4),))
    conv_out = normal_values(arg_keys[8], (TOKENS, D), 1.0, 6.0, ((0, 8), (1, 4)))
    gate_b = normal_values(arg_keys[9], (TOKENS, D), 1.0, 6.0, ((0, 8), (1, 4)))
    gate_c = normal_values(arg_keys[10], (TOKENS, D), 1.0, 6.0, ((0, 8), (1, 4)))
    value_v = normal_values(arg_keys[11], (TOKENS, D), 1.0, 6.0, ((0, 8), (1, 4)))
    conv_taps = normal_values(arg_keys[12], (3, D), 0.6, 3.0, ((1, 4),), jnp.float32)
    return {"out_grad": out_grad, "moe_input": moe_input, "route_weight": route_weight, "route_ids": route_ids, "gate_proj": gate_proj, "up_proj": up_proj, "down_proj": down_proj, "out_proj": out_proj, "conv_out": conv_out, "gate_b": gate_b, "gate_c": gate_c, "value_v": value_v, "conv_taps": conv_taps}


def slot_table(route_ids):
    flat = route_ids.reshape(N_SP, TOK_DEV * 2).astype(jnp.int32)
    onehot = (flat[:, :, None] == jnp.arange(EXPERTS, dtype=jnp.int32)[None, None, :]).astype(jnp.int32)
    before = jnp.cumsum(onehot, axis=1) - onehot
    slot = jnp.sum(before * onehot, axis=2).astype(jnp.int32)
    return (flat * CAP + slot).astype(jnp.int32)


def place_rows(rows, index):
    return jnp.zeros((EXPERTS * CAP, rows.shape[1]), rows.dtype).at[index].set(rows)


def reference(out_grad, moe_input, route_weight, route_ids, gate_proj, up_proj, down_proj, out_proj, conv_out, gate_b, gate_c, value_v, conv_taps):
    dest = slot_table(route_ids)
    sent = (route_weight[:, :, None] * out_grad.astype(jnp.float32)[:, None, :]).astype(jnp.bfloat16)
    rows_x = jnp.broadcast_to(moe_input[:, None, :], (TOKENS, 2, D)).reshape(N_SP, 2 * TOK_DEV, D)
    rows_dy = sent.reshape(N_SP, 2 * TOK_DEV, D)
    slots_x = jax.vmap(place_rows)(rows_x, dest).reshape(N_SP, EXPERTS, CAP, D)
    slots_dy = jax.vmap(place_rows)(rows_dy, dest).reshape(N_SP, EXPERTS, CAP, D)
    width = FF // N_TP

    def expert(index):
        xin = slots_x[:, index].reshape(N_SP * CAP, D)
        dyin = slots_dy[:, index].reshape(N_SP * CAP, D)
        w_gate = gate_proj[index]
        w_up = up_proj[index]
        w_down = down_proj[index]
        gate = jnp.dot(xin, w_gate, preferred_element_type=jnp.float32)
        upval = jnp.dot(xin, w_up, preferred_element_type=jnp.float32)
        sig = jax.nn.sigmoid(gate)
        act = gate * sig
        hidden = (act * upval).astype(jnp.bfloat16)
        g_down = jnp.dot(hidden.T, dyin, preferred_element_type=jnp.float32).astype(jnp.bfloat16)
        dhid = jnp.dot(dyin, w_down.T, preferred_element_type=jnp.float32)
        dgate = (dhid * upval * (sig * (1.0 + gate * (1.0 - sig)))).astype(jnp.bfloat16)
        dup = (dhid * act).astype(jnp.bfloat16)
        g_gate = jnp.dot(xin.T, dgate, preferred_element_type=jnp.float32).astype(jnp.bfloat16)
        g_up = jnp.dot(xin.T, dup, preferred_element_type=jnp.float32).astype(jnp.bfloat16)
        rows = N_SP * CAP
        part = jnp.einsum('rpf,dpf->prd', dgate.reshape(rows, N_TP, width).astype(jnp.float32),
                          w_gate.reshape(D, N_TP, width).astype(jnp.float32))
        part = part + jnp.einsum('rpf,dpf->prd', dup.reshape(rows, N_TP, width).astype(jnp.float32),
                                 w_up.reshape(D, N_TP, width).astype(jnp.float32))
        part = lax.optimization_barrier(part.astype(jnp.bfloat16)).astype(jnp.float32)
        back = jnp.sum(part, axis=0).astype(jnp.bfloat16)
        return g_gate, g_up, g_down, back

    grad_gate, grad_up, grad_down, backs = lax.map(expert, jnp.arange(EXPERTS, dtype=jnp.int32))
    backs = backs.reshape(EXPERTS, N_SP, CAP, D).transpose(1, 0, 2, 3).reshape(N_SP, EXPERTS * CAP, D)
    picked = jax.vmap(lambda table, index: table[index])(backs, dest)
    moe_grad = jnp.sum(picked.reshape(TOKENS, 2, D).astype(jnp.float32), axis=1)
    grad_h = (out_grad.astype(jnp.float32) + moe_grad).astype(jnp.bfloat16)
    grad_z = jnp.dot(grad_h, out_proj, preferred_element_type=jnp.float32)
    dconv = (grad_z * gate_b.astype(jnp.float32)).astype(jnp.bfloat16)
    grad_b = (grad_z * conv_out.astype(jnp.float32)).astype(jnp.bfloat16)
    padded = jnp.pad(dconv.astype(jnp.float32), ((1, 1), (0, 0)))
    grad_u = conv_taps[0] * padded[2:] + conv_taps[1] * padded[1:-1] + conv_taps[2] * padded[:-2]
    grad_c = (grad_u * value_v.astype(jnp.float32)).astype(jnp.bfloat16)
    grad_v = (grad_u * gate_c.astype(jnp.float32)).astype(jnp.bfloat16)
    mixed = (gate_b.astype(jnp.float32) * conv_out.astype(jnp.float32)).astype(jnp.bfloat16)
    grad_out = jnp.dot(grad_h.T, mixed, preferred_element_type=jnp.float32)
    return grad_gate, grad_up, grad_down, grad_out, grad_b, grad_c, grad_v
```

```python
import functools

import jax
import jax.numpy as jnp
from jax import lax
from jax.experimental import pallas as pl
from jax.experimental.pallas import tpu as pltpu
from jax.sharding import PartitionSpec as P

MESH = pl.DeviceIdType.MESH
HALF = jnp.bfloat16
F32 = jnp.float32
PLAIN = (((1,), (0,)), ((), ()))
RIGHT_T = (((1,), (1,)), ((), ()))


def remote(src, dst, send_sem, recv_sem, device):
    return pltpu.make_async_remote_copy(
        src_ref=src,
        dst_ref=dst,
        send_sem=send_sem,
        recv_sem=recv_sem,
        device_id=device,
        device_id_type=MESH,
    )


def offsets(n):
    m = n // 2
    shifts = [0] + sorted(range(1, m), key=lambda k: -min(k, m - k))
    return [(k, f) for k in shifts for f in range(2)]


def layer_kernel(
    n, q,
    ids_hbm, rw_hbm, x_hbm, g_hbm, b_hbm, co_hbm, c_hbm, v_hbm, taps_hbm,
    wg_hbm, wu_hbm, wd_hbm, wo_hbm,
    gout_ref, gb_ref, gc_ref, gv_ref, ggate_ref, gup_ref, gdown_ref,
    ids_ref, rw_ref, x_ref, g_ref, b_ref, co_ref, c_ref, v_ref, taps_ref,
    wg, wu, wd, wo, p01, p_ref, p_t, send, buf, gate, upval, dhid, hid, dg, du, turned,
    part, rsib, pair, ryb, fin, ret, full_h, h_t, all_t, all_m, edge, got, padded,
    w_sem,
    s1, r1, sy, ry, ss, rs, s2, r2, s3, r3, s4, r4,
    sm, rm, sp, rp, shy, rhy, shs, rhs, sa, ra, sf, rf, se, re,
):
    s, t = lax.axis_index("sp"), lax.axis_index("tp")
    core = lax.rem(t, 2)
    sibling = t + 1 - 2 * core
    partner = s + 1 - 2 * lax.rem(s, 2)
    ny = q // 2
    tok, cols = x_ref.shape
    total, width = part.shape
    cap = total // n
    share = width // n
    units = wg.shape[0]
    pairs = offsets(n)
    batch = total // 2
    mid = n // 2

    barrier = pltpu.get_barrier_semaphore()
    for i in range(1, n):
        pl.semaphore_signal(
            barrier, inc=1, device_id=(lax.rem(s + i, n), t), device_id_type=MESH
        )
    for d in range(1, ny):
        pl.semaphore_signal(
            barrier, inc=1, device_id=(s, lax.rem(t + 2 * d, q)), device_id_type=MESH
        )
    pl.semaphore_signal(barrier, inc=1, device_id=(s, sibling), device_id_type=MESH)

    loads = [
        pltpu.make_async_copy(source, target, w_sem.at[k])
        for k, (source, target) in enumerate(
            zip(
                (
                    wg_hbm, wu_hbm, wd_hbm, wo_hbm, ids_hbm, x_hbm, rw_hbm, g_hbm,
                    b_hbm, co_hbm, c_hbm, v_hbm, taps_hbm,
                ),
                (
                    wg, wu, wd, wo, ids_ref, x_ref, rw_ref, g_ref,
                    b_ref, co_ref, c_ref, v_ref, taps_ref,
                ),
            )
        )
    ]
    for load in [*loads[4:], *loads[:4]]:
        load.start()

    def to(p):
        k, f = pairs[p]
        return lax.rem((partner if f else s) + 2 * k, n)

    def source(p):
        k, f = pairs[p]
        return lax.rem((partner if f else s) - 2 * k + n, n)

    def rows(p):
        return slice(p * cap, (p + 1) * cap)

    def at_cols(tt):
        return pl.ds(pl.multiple_of(tt * cols, cols), cols)

    loads[4].wait()
    ids0, ids1 = ids_ref[0:1, :], ids_ref[1:2, :]
    where = lax.broadcasted_iota(jnp.int32, (n, tok), 0)
    experts = jnp.zeros((n, tok), jnp.int32)
    for p in range(n):
        experts = jnp.where(where == p, to(p), experts)
    named = jnp.logical_or(ids0 == experts, ids1 == experts)
    row_i = lax.broadcasted_iota(jnp.int32, (tok, tok), 0)
    col_i = lax.broadcasted_iota(jnp.int32, (tok, tok), 1)
    before = jnp.dot(
        jnp.where(named, 1.0, 0.0).astype(HALF),
        jnp.where(row_i < col_i, 1.0, 0.0).astype(HALF),
        preferred_element_type=F32,
    ).astype(jnp.int32)
    slots = lax.broadcasted_iota(jnp.int32, (cap, tok), 0)
    for p in range(n):
        here = before[p : p + 1, :] == slots
        c0 = jnp.where(jnp.logical_and(here, ids0 == to(p)), 1.0, 0.0)
        c1 = jnp.where(jnp.logical_and(here, ids1 == to(p)), 1.0, 0.0)
        p01[rows(p), 0:tok] = c0.astype(HALF)
        p01[rows(p), tok : 2 * tok] = c1.astype(HALF)
        p_ref[rows(p), :] = (c0 + c1).astype(HALF)

    def first(a, p):
        return remote(
            send.at[a, rows(p)],
            buf.at[a, rows(p), at_cols(t)],
            s1.at[a, p],
            r1.at[a, p],
            (to(p), t),
        )

    def across(a, p, d):
        b = buf.at[a, rows(p), at_cols(t)]
        return remote(
            b, b, sy.at[a, p, d - 1], ry.at[a, p, d - 1], (s, lax.rem(t + 2 * d, q))
        )

    def beside(a, p, d):
        b = buf.at[a, rows(p), at_cols(lax.rem(t - 2 * d + q, q))]
        return remote(b, b, ss.at[a, p, d], rs.at[a, p, d], (s, sibling))

    send_order = [*range(2, n), 1]
    loads[5].wait()
    send[0] = jnp.dot(p_ref[...], x_ref[...], preferred_element_type=F32).astype(HALF)
    pl.semaphore_wait(barrier, n - 1 + ny)
    for p in send_order:
        first(0, p).start()
    buf[0, rows(0), at_cols(t)] = send[0, rows(0), :]
    loads[6].wait()
    loads[7].wait()
    grad = g_ref[...].astype(F32)
    weighted = []
    for k in range(2):
        column = jnp.sum(
            jnp.where(row_i == col_i, rw_ref[k : k + 1, :], 0.0), axis=1, keepdims=True
        )
        weighted.append((column * grad).astype(HALF))
    send[1] = jnp.dot(
        p01[...], jnp.concatenate(weighted, axis=0), preferred_element_type=F32
    ).astype(HALF)
    for p in send_order:
        first(1, p).start()
    buf[1, rows(0), at_cols(t)] = send[1, rows(0), :]

    def span(h):
        return slice(h * batch, (h + 1) * batch)

    def forward_gate(h):
        gate[span(h), :] = lax.dot_general(
            buf[0, span(h), :], wg[...], RIGHT_T, preferred_element_type=F32
        )

    def forward_up(h):
        upval[span(h), :] = lax.dot_general(
            buf[0, span(h), :], wu[...], RIGHT_T, preferred_element_type=F32
        )

    def back_hidden(h):
        dhid[span(h), :] = lax.dot_general(
            buf[1, span(h), :], wd[...], RIGHT_T, preferred_element_type=F32
        )

    step_rows = 32

    def activation(h):
        def step(r, _):
            at = pl.ds(pl.multiple_of(h * batch + r * step_rows, step_rows), step_rows)
            z, u, dh = gate[at, :], upval[at, :], dhid[at, :]
            sig = jax.nn.sigmoid(z)
            act = z * sig
            hid[at, :] = (act * u).astype(HALF)
            dg[at, :] = (dh * u * (sig * (1.0 + z * (1.0 - sig)))).astype(HALF)
            du[at, :] = (dh * act).astype(HALF)
            return 0

        lax.fori_loop(0, batch // step_rows, step, 0)

    def partial(h):
        def step(k, _):
            here = at_cols(k)
            part[span(h), here] = (
                lax.dot_general(
                    dg[span(h), :], wg[:, here], PLAIN, preferred_element_type=F32
                )
                + lax.dot_general(
                    du[span(h), :], wu[:, here], PLAIN, preferred_element_type=F32
                )
            ).astype(HALF)
            return 0

        lax.fori_loop(0, q, step, 0)

    seq = [(0, 0), (1, 0), (0, 1), (1, 1)]
    seq += [(0, p) for p in range(2, n)] + [(1, p) for p in range(2, n)]

    def last_of(a, h):
        return max(k for k, (b, p) in enumerate(seq) if b == a and p // mid == h)

    drained = set()

    def drain(upto):
        for k in range(upto + 1):
            if k not in drained:
                drained.add(k)
                for d in range(ny):
                    beside(*seq[k], d).wait_recv()

    def weights(k):
        loads[k].wait()

    def mixed_own():
        for k in range(8, 13):
            loads[k].wait()
        all_m[0:tok, :] = (b_ref[...].astype(F32) * co_ref[...].astype(F32)).astype(HALF)

    def turn_slots():
        p_t[...] = p_ref[...].astype(F32).T.astype(HALF)

    hooks = {}

    def hook(k, *calls):
        hooks.setdefault(min(k, len(seq) - 1), []).extend(calls)

    hook(1, (None, mixed_own))
    hook(2, (None, turn_slots))
    x_a, x_b = last_of(0, 0), last_of(0, 1)
    d_a, d_b = last_of(1, 0), last_of(1, 1)
    hook(x_a + 3, (x_a, lambda: (weights(0), forward_gate(0))))
    hook(x_a + 4, (x_a, lambda: (weights(1), forward_up(0))))
    hook(x_b + 3, (x_b, lambda: forward_gate(1)))
    hook(x_b + 4, (x_b, lambda: forward_up(1)))
    hook(d_a + 3, (d_a, lambda: (weights(2), back_hidden(0))))
    hook(d_a + 4, (d_a, lambda: activation(0)))

    def forward(k):
        for d in range(1, ny):
            across(*seq[k], d).wait_recv()
            beside(*seq[k], d).start()

    for k, (a, p) in enumerate(seq):
        if p:
            first(a, p).wait_recv()
        for d in range(1, ny):
            across(a, p, d).start()
        beside(a, p, 0).start()
        if k:
            forward(k - 1)
        for need, call in hooks.get(k, []):
            if need is not None:
                drain(need)
            call()

    def mixed_far(k):
        return remote(
            all_m.at[0:tok],
            all_m.at[slot_of(k, 0)],
            sm.at[k],
            rm.at[k],
            (lax.rem(s + 2 * k, n), t),
        )

    def slot_of(k, f):
        p = pairs.index((k, f))
        return slice(p * tok, (p + 1) * tok)

    def mixed_near(k):
        return remote(
            all_m.at[slot_of(k, 0)], all_m.at[slot_of(k, 1)], sp.at[k], rp.at[k], (partner, t)
        )

    def to_side(p, d):
        theirs = lax.rem(sibling + 2 * d, q)
        return remote(
            part.at[rows(p), at_cols(theirs)],
            rsib.at[d, rows(p)],
            s2.at[p, d],
            r2.at[p, d],
            (s, sibling),
        )

    def to_far(p, d):
        return remote(
            pair.at[d - 1, rows(p)],
            ryb.at[d - 1, rows(p)],
            s3.at[p, d - 1],
            r3.at[p, d - 1],
            (s, lax.rem(t + 2 * d, q)),
        )

    def back(p):
        return remote(fin.at[rows(p)], ret.at[rows(p)], s4.at[p], r4.at[p], (source(p), t))

    def mine(p, d):
        value = part[rows(p), at_cols(lax.rem(t + 2 * d, q))].astype(F32)
        return value + rsib[d, rows(p), :].astype(F32)

    def side_start(p):
        for d in [*range(1, ny), 0]:
            to_side(p, d).start()

    def pair_up(p):
        for d in range(1, ny):
            to_side(p, d).wait_recv()
            pair[d - 1, rows(p), :] = mine(p, d).astype(HALF)
            to_far(p, d).start()

    def finish(p):
        to_side(p, 0).wait_recv()
        value = mine(p, 0)
        for d in range(1, ny):
            to_far(p, d).wait_recv()
            value = value + ryb[d - 1, rows(p), :].astype(F32)
        if p:
            fin[rows(p), :] = value.astype(HALF)
            back(p).start()
        else:
            ret[rows(p), :] = value.astype(HALF)

    near_half, far_half = [*range(2, mid), 1, 0], [*range(mid, n)]
    forward(len(seq) - 1)
    shifts = [k for k, f in pairs if f == 0][1:]
    early, late = shifts[: (len(shifts) + 1) // 3], shifts[(len(shifts) + 1) // 3 :]
    for k in early:
        mixed_far(k).start()
    mixed_near(0).start()
    partial(0)
    for p in near_half:
        side_start(p)
    drain(d_b)
    back_hidden(1)
    for p in near_half[:-1]:
        pair_up(p)
    activation(1)
    finish(near_half[0])
    partial(1)
    for p in far_half:
        side_start(p)
    if len(near_half) > 2:
        finish(near_half[1])
    for p in far_half + [0]:
        pair_up(p)
    for p in near_half[2:-1] + far_half + [0]:
        finish(p)
    for k in early:
        mixed_far(k).wait_recv()
        mixed_near(k).start()
    for k in late:
        mixed_far(k).start()

    def weight_grad(left, a, target):
        turned[...] = left[...].astype(F32).T.astype(HALF)

        def step(j, _):
            here = at_cols(j)
            target[:, here] = lax.dot_general(
                turned[...], buf[a, :, here], PLAIN, preferred_element_type=F32
            ).astype(HALF)
            return 0

        lax.fori_loop(0, q, step, 0)

    weight_grad(hid, 1, gdown_ref)
    for p in range(1, n):
        back(p).wait_recv()
    moe = jnp.dot(p_t[...], ret[...], preferred_element_type=F32)
    full_h[:, at_cols(t)] = (g_ref[...].astype(F32) + moe).astype(HALF)

    def h_across(d):
        b = full_h.at[:, at_cols(t)]
        return remote(b, b, shy.at[d - 1], rhy.at[d - 1], (s, lax.rem(t + 2 * d, q)))

    def h_beside(d):
        b = full_h.at[:, at_cols(lax.rem(t - 2 * d + q, q))]
        return remote(b, b, shs.at[d], rhs.at[d], (s, sibling))

    for d in range(1, ny):
        h_across(d).start()
    h_beside(0).start()

    def turn_h(tt):
        h_t[at_cols(tt), :] = full_h[:, at_cols(tt)].astype(F32).T.astype(HALF)

    turn_h(t)
    weights(3)
    weight_grad(dg, 0, ggate_ref)
    h_beside(0).wait_recv()
    turn_h(sibling)
    for d in range(1, ny):
        h_across(d).wait_recv()
        h_beside(d).start()
        turn_h(lax.rem(t - 2 * d + q, q))
    for d in range(1, ny):
        h_beside(d).wait_recv()
        turn_h(lax.rem(sibling - 2 * d + q, q))

    part_share = share // 2

    def half_rows(first_row):
        return pl.ds(
            pl.multiple_of(first_row + core * part_share, part_share), part_share
        )

    def tokens(p):
        return slice(p * tok, (p + 1) * tok)

    def h_far(p):
        return remote(
            h_t.at[half_rows(to(p) * share)],
            all_t.at[half_rows(0), tokens(p)],
            sa.at[p],
            ra.at[p],
            (to(p), t),
        )

    def h_pass(p):
        b = all_t.at[half_rows(0), tokens(p)]
        return remote(b, b, sf.at[p], rf.at[p], (s, sibling))

    for p in send_order:
        h_far(p).start()
    all_t[:, tokens(0)] = h_t[pl.ds(pl.multiple_of(s * share, share), share), :]

    def halo(k):
        there = lax.rem(s + 1, n) if k == 0 else lax.rem(s - 1 + n, n)
        return remote(edge.at[k], got.at[k], se.at[k], re.at[k], (there, t))

    grad_z = jnp.dot(full_h[...], wo[...], preferred_element_type=F32)
    dconv = (grad_z * b_ref[...].astype(F32)).astype(HALF).astype(F32)
    edge[0] = jnp.broadcast_to(dconv[tok - 1 : tok, :], (8, cols))
    edge[1] = jnp.broadcast_to(dconv[0:1, :], (8, cols))
    halo(0).start()
    halo(1).start()
    gb_ref[...] = (grad_z * co_ref[...].astype(F32)).astype(HALF)
    padded[8 : 8 + tok, :] = dconv
    for k in late:
        mixed_far(k).wait_recv()
        mixed_near(k).start()
    weight_grad(du, 0, gup_ref)
    halo(0).wait_recv()
    halo(1).wait_recv()
    padded[0:8, :] = jnp.where(s > 0, got[0], 0.0)
    padded[8 + tok : 16 + tok, :] = jnp.where(s < n - 1, got[1], 0.0)
    grad_u = (
        taps_ref[0:1, :] * padded[9 : 9 + tok, :]
        + taps_ref[1:2, :] * padded[8 : 8 + tok, :]
        + taps_ref[2:3, :] * padded[7 : 7 + tok, :]
    )
    gc_ref[...] = (grad_u * v_ref[...].astype(F32)).astype(HALF)
    gv_ref[...] = (grad_u * c_ref[...].astype(F32)).astype(HALF)
    for p in send_order:
        h_far(p).wait_recv()
        h_pass(p).start()
    for k in [0, *early, *late]:
        mixed_near(k).wait_recv()
    for p in send_order:
        h_pass(p).wait_recv()
    gout_ref[...] = jnp.dot(all_t[...], all_m[...], preferred_element_type=F32)

    for p in range(n):
        for a in range(2):
            if p:
                first(a, p).wait_send()
            for d in range(1, ny):
                across(a, p, d).wait_send()
            for d in range(ny):
                beside(a, p, d).wait_send()
        for d in range(ny):
            to_side(p, d).wait_send()
            if d:
                to_far(p, d).wait_send()
        if p:
            back(p).wait_send()
            h_far(p).wait_send()
            h_pass(p).wait_send()
    for d in range(ny):
        if d:
            h_across(d).wait_send()
        h_beside(d).wait_send()
    for k in [0, *early, *late]:
        if k:
            mixed_far(k).wait_send()
        mixed_near(k).wait_send()
    halo(0).wait_send()
    halo(1).wait_send()


def layer(n, q, ids_t, weight_t, x, g, b, co, c, v, taps, wg, wu, wd, wo):
    tok, cols = x.shape
    units, width = wg.shape
    total = 4 * tok
    share = width // n
    ny = q // 2
    far = max(ny - 1, 1)
    vmem = pl.BlockSpec(memory_space=pltpu.VMEM)
    hbm = pl.BlockSpec(memory_space=pltpu.HBM)
    dma = pltpu.SemaphoreType.DMA
    like = pltpu.VMEM(g.shape, HALF)
    tall = pltpu.VMEM((units, width), HALF)

    def half(*shape):
        return pltpu.VMEM(shape, HALF)

    def full(*shape):
        return pltpu.VMEM(shape, F32)

    sems = [
        (2, n), (2, n, far), (2, n, ny), (n, ny), (n, far), (n,),
        (n // 2,), (n // 2,), (far,), (ny,), (n,), (n,), (2,),
    ]
    return pl.pallas_call(
        functools.partial(layer_kernel, n, q),
        out_shape=(
            pltpu.VMEM((share, cols), F32), like, like, like, tall, tall, tall,
        ),
        in_specs=[hbm] * 13,
        out_specs=(vmem,) * 7,
        scratch_shapes=[
            pltpu.VMEM(ids_t.shape, ids_t.dtype),
            full(*weight_t.shape),
            half(tok, cols),
            half(tok, cols),
            half(tok, cols),
            half(tok, cols),
            half(tok, cols),
            half(tok, cols),
            full(*taps.shape),
            half(units, width),
            half(units, width),
            half(units, width),
            half(width, cols),
            half(total, 2 * tok),
            half(total, tok),
            half(tok, total),
            half(2, total, cols),
            half(2, total, width),
            full(total, units),
            full(total, units),
            full(total, units),
            half(total, units),
            half(total, units),
            half(total, units),
            half(units, total),
            half(total, width),
            half(ny, total, cols),
            half(far, total, cols),
            half(far, total, cols),
            half(total, cols),
            half(total, cols),
            half(tok, width),
            half(width, tok),
            half(share, n * tok),
            half(n * tok, cols),
            full(2, 8, cols),
            full(2, 8, cols),
            full(tok + 16, cols),
            dma((13,)),
        ]
        + [dma(shape) for shape in sems for _ in range(2)],
        compiler_params=pltpu.CompilerParams(
            collective_id=0, has_side_effects=True, vmem_limit_bytes=44 * 2**20
        ),
        name="layer",
    )(
        *(
            pltpu.with_memory_space_constraint(a, pltpu.HBM)
            for a in (ids_t, weight_t, x, g, b, co, c, v, taps, wg, wu, wd, wo)
        )
    )


def settle_kernel(*refs):
    count = (len(refs) - 1) // 2
    sem = refs[-1]
    copies = [
        pltpu.make_async_copy(refs[k], refs[count + k], sem.at[k]) for k in range(count)
    ]
    for copy in copies:
        copy.start()
    for copy in copies:
        copy.wait()


def settle(*arrays):
    return pl.pallas_call(
        settle_kernel,
        out_shape=tuple(pltpu.HBM(a.shape, a.dtype) for a in arrays),
        in_specs=[pl.BlockSpec(memory_space=pltpu.VMEM)] * len(arrays),
        out_specs=(pl.BlockSpec(memory_space=pltpu.HBM),) * len(arrays),
        scratch_shapes=[pltpu.SemaphoreType.DMA((len(arrays),))],
        compiler_params=pltpu.CompilerParams(vmem_limit_bytes=2**20),
        name="settle",
    )(*(pltpu.with_memory_space_constraint(a, pltpu.VMEM) for a in arrays))


def local(
    out_grad,
    moe_input,
    route_weight,
    route_ids,
    gate_proj,
    up_proj,
    down_proj,
    out_proj,
    conv_out,
    gate_b,
    gate_c,
    value_v,
    conv_taps,
):
    n = lax.axis_size("sp")
    q = lax.axis_size("tp")
    results = layer(
        n, q, route_ids.T, route_weight.T, moe_input, out_grad, gate_b, conv_out, gate_c,
        value_v, conv_taps, gate_proj[0].T, up_proj[0].T, down_proj[0], out_proj,
    )
    grad_out, grad_b, grad_c, grad_v, grad_gate, grad_up, grad_down = settle(*results)
    return (grad_gate.T[None], grad_up.T[None], grad_down[None], grad_out, grad_b, grad_c, grad_v)


def solution(mesh):
    in_specs = (
        P("sp", "tp"),
        P("sp", "tp"),
        P("sp", None),
        P("sp", None),
        P("sp", None, "tp"),
        P("sp", None, "tp"),
        P("sp", "tp", None),
        P(None, "tp"),
        P("sp", "tp"),
        P("sp", "tp"),
        P("sp", "tp"),
        P("sp", "tp"),
        P(None, "tp"),
    )
    out_specs = (
        P("sp", None, "tp"),
        P("sp", None, "tp"),
        P("sp", "tp", None),
        P("sp", "tp"),
        P("sp", "tp"),
        P("sp", "tp"),
        P("sp", "tp"),
    )
    return jax.shard_map(local, mesh=mesh, in_specs=in_specs, out_specs=out_specs, check_vma=False)
```

```python
import functools

import jax
import jax.numpy as jnp
from jax import lax
from jax.experimental import pallas as pl
from jax.experimental.pallas import tpu as pltpu
from jax.sharding import PartitionSpec as P

MESH = pl.DeviceIdType.MESH
HALF = jnp.bfloat16
F32 = jnp.float32
PLAIN = (((1,), (0,)), ((), ()))
RIGHT_T = (((1,), (1,)), ((), ()))


def remote(src, dst, send_sem, recv_sem, device):
    return pltpu.make_async_remote_copy(
        src_ref=src,
        dst_ref=dst,
        send_sem=send_sem,
        recv_sem=recv_sem,
        device_id=device,
        device_id_type=MESH,
    )


def layer_kernel(
    n, q,
    ids_hbm, rw_hbm, x_hbm, g_hbm, b_hbm, co_hbm, c_hbm, v_hbm, taps_hbm,
    wg_hbm, wu_hbm, wd_hbm, wo_hbm,
    gout_ref, gb_ref, gc_ref, gv_ref, ggate_ref, gup_ref, gdown_ref,
    ids_ref, rw_ref, x_ref, g_ref, b_ref, co_ref, c_ref, v_ref, taps_ref,
    wg, wu, wd, wo, ids_in, rw_in, x_in, g_in, p01, p_in, p_ref, p_t, send, send_in, buf, gate, upval, dhid, hid, dg, du, turned,
    part, rsib, pair, ryb, fin, ret, full_h, h_t, all_t, all_m, edge, got, padded,
    w_sem, st, rt,
    s1, r1, sy, ry, ss, rs, s2, r2, s3, r3, s4, r4,
    sm, rm, shy, rhy, shs, rhs, sa, ra, sf, rf, se, re,
):
    s, t = lax.axis_index("sp"), lax.axis_index("tp")
    core = lax.rem(t, 2)
    sibling = t + 1 - 2 * core
    ny = q // 2
    tok, cols = x_ref.shape
    total, width = part.shape
    cap = total // n
    share = width // n
    units = wg.shape[0]
    top = n // 2
    batch = total // 2

    barrier = pltpu.get_barrier_semaphore()
    for i in range(1, n):
        pl.semaphore_signal(
            barrier, inc=1, device_id=(lax.rem(s + i, n), t), device_id_type=MESH
        )
    for d in range(1, ny):
        pl.semaphore_signal(
            barrier, inc=1, device_id=(s, lax.rem(t + 2 * d, q)), device_id_type=MESH
        )
    pl.semaphore_signal(barrier, inc=1, device_id=(s, sibling), device_id_type=MESH)

    loads = [
        pltpu.make_async_copy(source, target, w_sem.at[k])
        for k, (source, target) in enumerate(
            zip(
                (
                    wg_hbm, wu_hbm, wd_hbm, wo_hbm, ids_hbm, x_hbm, rw_hbm, g_hbm,
                    b_hbm, co_hbm, c_hbm, v_hbm, taps_hbm,
                ),
                (
                    wg, wu, wd, wo, ids_ref, x_ref, rw_ref, g_ref,
                    b_ref, co_ref, c_ref, v_ref, taps_ref,
                ),
            )
        )
    ]
    for load in [*loads[4:], *loads[:4]]:
        load.start()

    def peer(k):
        value = s
        for b in range(n.bit_length() - 1):
            if k >> b & 1:
                value = value + (1 - 2 * lax.rem(lax.div(s, 1 << b), 2)) * (1 << b)
        return value

    def rows(k):
        p = k ^ top
        return slice(p * cap, (p + 1) * cap)

    def near_rows(k):
        return slice(k * cap, (k + 1) * cap)

    def at_cols(tt):
        return pl.ds(pl.multiple_of(tt * cols, cols), cols)

    row_i = lax.broadcasted_iota(jnp.int32, (tok, tok), 0)
    col_i = lax.broadcasted_iota(jnp.int32, (tok, tok), 1)
    slots = lax.broadcasted_iota(jnp.int32, (cap, tok), 0)

    def choices(ids, ks):
        ids0, ids1 = ids[0:1, :], ids[1:2, :]
        where = lax.broadcasted_iota(jnp.int32, (n, tok), 0)
        experts = jnp.full((n, tok), -1, jnp.int32)
        for i, k in enumerate(ks):
            experts = jnp.where(where == i, peer(k), experts)
        named = jnp.logical_or(ids0 == experts, ids1 == experts)
        before = jnp.dot(
            jnp.where(named, 1.0, 0.0).astype(HALF),
            jnp.where(row_i < col_i, 1.0, 0.0).astype(HALF),
            preferred_element_type=F32,
        ).astype(jnp.int32)
        for i, k in enumerate(ks):
            here = before[i : i + 1, :] == slots
            c0 = jnp.where(jnp.logical_and(here, ids0 == peer(k)), 1.0, 0.0)
            c1 = jnp.where(jnp.logical_and(here, ids1 == peer(k)), 1.0, 0.0)
            yield k, c0, c1

    def weighted(rw, g):
        grad = g[...].astype(F32)
        parts = []
        for k in range(2):
            column = jnp.sum(
                jnp.where(row_i == col_i, rw[k : k + 1, :], 0.0), axis=1, keepdims=True
            )
            parts.append((column * grad).astype(HALF))
        return jnp.concatenate(parts, axis=0)

    def tokens_out(i):
        here, there = ((ids_ref, ids_in), (x_ref, x_in), (rw_ref, rw_in), (g_ref, g_in))[i]
        return remote(here, there, st.at[i], rt.at[i], (peer(top), t))

    def first(a, k):
        if k < top:
            rows_out = send.at[a, near_rows(k)]
        else:
            rows_out = send_in.at[a, near_rows(k ^ top)]
        return remote(
            rows_out,
            buf.at[a, rows(k), at_cols(t)],
            s1.at[a, k],
            r1.at[a, k],
            (peer(k % top), t),
        )

    def across(a, p, d):
        b = buf.at[a, rows(p), at_cols(t)]
        return remote(
            b, b, sy.at[a, p, d - 1], ry.at[a, p, d - 1], (s, lax.rem(t + 2 * d, q))
        )

    def beside(a, p, d):
        b = buf.at[a, rows(p), at_cols(lax.rem(t - 2 * d + q, q))]
        return remote(b, b, ss.at[a, p, d], rs.at[a, p, d], (s, sibling))

    near = [*range(1, top)]
    own_ks, rest_ks = [*range(top // 2)], [*range(top // 2, top)]
    far_ks = [*range(top, n)]

    loads[4].wait()
    loads[5].wait()
    pl.semaphore_wait(barrier, n - 1 + ny)
    tokens_out(0).start()
    tokens_out(1).start()
    for k, c0, c1 in choices(ids_ref, range(top)):
        p01[near_rows(k), 0:tok] = c0.astype(HALF)
        p01[near_rows(k), tok : 2 * tok] = c1.astype(HALF)
        p_ref[rows(k), :] = (c0 + c1).astype(HALF)
    send[0] = jnp.dot(
        p_ref[batch:total, :], x_ref[...], preferred_element_type=F32
    ).astype(HALF)
    for k in near:
        first(0, k).start()
    buf[0, rows(0), at_cols(t)] = send[0, near_rows(0), :]
    loads[6].wait()
    loads[7].wait()
    tokens_out(2).start()
    tokens_out(3).start()
    send[1] = jnp.dot(
        p01[...], weighted(rw_ref, g_ref), preferred_element_type=F32
    ).astype(HALF)
    for k in own_ks[1:]:
        first(1, k).start()
    buf[1, rows(0), at_cols(t)] = send[1, near_rows(0), :]

    def sort_x():
        tokens_out(0).wait_recv()
        tokens_out(1).wait_recv()
        for k, c0, c1 in choices(ids_in, range(top)):
            p01[near_rows(k), 0:tok] = c0.astype(HALF)
            p01[near_rows(k), tok : 2 * tok] = c1.astype(HALF)
            p_in[near_rows(k), :] = (c0 + c1).astype(HALF)
        send_in[0] = jnp.dot(
            p_in[...], x_in[...], preferred_element_type=F32
        ).astype(HALF)
        for k in near:
            first(0, k ^ top).start()
        buf[0, rows(top), at_cols(t)] = send_in[0, near_rows(0), :]

    def sort_g():
        tokens_out(2).wait_recv()
        tokens_out(3).wait_recv()
        send_in[1] = jnp.dot(
            p01[...], weighted(rw_in, g_in), preferred_element_type=F32
        ).astype(HALF)
        for k in near:
            first(1, k ^ top).start()
        for k in rest_ks:
            first(1, k).start()
        buf[1, rows(top), at_cols(t)] = send_in[1, near_rows(0), :]

    def span(h):
        return slice(h * batch, (h + 1) * batch)

    def forward_gate(h):
        gate[span(h), :] = lax.dot_general(
            buf[0, span(h), :], wg[...], RIGHT_T, preferred_element_type=F32
        )

    def forward_up(h):
        upval[span(h), :] = lax.dot_general(
            buf[0, span(h), :], wu[...], RIGHT_T, preferred_element_type=F32
        )

    def back_hidden(at):
        dhid[at, :] = lax.dot_general(
            buf[1, at, :], wd[...], RIGHT_T, preferred_element_type=F32
        )

    step_rows = 32

    def activation(span_at):
        def step(r, _):
            at = pl.ds(
                pl.multiple_of(span_at.start + r * step_rows, step_rows), step_rows
            )
            z, u, dh = gate[at, :], upval[at, :], dhid[at, :]
            sig = jax.nn.sigmoid(z)
            act = z * sig
            hid[at, :] = (act * u).astype(HALF)
            dg[at, :] = (dh * u * (sig * (1.0 + z * (1.0 - sig)))).astype(HALF)
            du[at, :] = (dh * act).astype(HALF)
            return 0

        lax.fori_loop(0, (span_at.stop - span_at.start) // step_rows, step, 0)

    def partial(at):
        def step(k, _):
            here = at_cols(k)
            part[at, here] = (
                lax.dot_general(
                    dg[at, :], wg[:, here], PLAIN, preferred_element_type=F32
                )
                + lax.dot_general(
                    du[at, :], wu[:, here], PLAIN, preferred_element_type=F32
                )
            ).astype(HALF)
            return 0

        lax.fori_loop(0, q, step, 0)

    far_rows = slice(0, batch)
    far_halves = [slice(0, batch // 2), slice(batch // 2, batch)]
    own_rows = slice(batch, batch + batch // 2)
    rest_rows = slice(batch + batch // 2, total)
    seq = [(a, k) for k in own_ks for a in range(2)]
    seq += [(0, k) for k in rest_ks + far_ks] + [(1, k) for k in far_ks + rest_ks]
    lag = 3
    forwarded, drained = set(), set()

    def forward(upto):
        for k in range(upto + 1):
            if k not in forwarded:
                forwarded.add(k)
                for d in range(1, ny):
                    across(*seq[k], d).wait_recv()
                    beside(*seq[k], d).start()

    def drain(upto):
        forward(upto)
        for k in range(upto + 1):
            if k not in drained:
                drained.add(k)
                for d in range(ny):
                    beside(*seq[k], d).wait_recv()

    def weights(k):
        loads[k].wait()

    def tokens(k):
        p = k ^ top
        return slice(p * tok, (p + 1) * tok)

    def mixed(k):
        low = k & -k
        return remote(
            all_m.at[tokens(k ^ low)], all_m.at[tokens(k)], sm.at[k], rm.at[k], (peer(low), t)
        )

    def mixed_own():
        for k in range(8, 13):
            loads[k].wait()
        all_m[tokens(0), :] = (b_ref[...].astype(F32) * co_ref[...].astype(F32)).astype(HALF)

    def mixed_stage(low):
        for k in range(0, n, 2 * low):
            if k & -k == 2 * low:
                mixed(k).wait_recv()
        for k in range(low, n, 2 * low):
            mixed(k).start()

    def turn_slots():
        for k, c0, c1 in choices(ids_ref, far_ks):
            p_ref[rows(k), :] = (c0 + c1).astype(HALF)
        p_t[...] = p_ref[...].astype(F32).T.astype(HALF)

    ahead, hooks = {}, {}

    def hook(k, *calls):
        hooks.setdefault(min(k, len(seq) - 1), []).extend(calls)

    at = {unit: k for k, unit in enumerate(seq)}
    x_own, x_far = at[0, top - 1], at[0, n - 1]
    ahead[at[0, rest_ks[-1]]] = sort_x
    ahead[at[0, top + 1]] = sort_g
    hook(1, mixed_own)
    hook(3, turn_slots)
    hook(x_own + 3, lambda: (drain(x_own), weights(0), forward_gate(1)))
    hook(x_own + 4, lambda: (weights(1), forward_up(1)))
    hook(x_own + 5, lambda: (weights(2), back_hidden(own_rows), activation(own_rows)))
    hook(x_far + 3, lambda: (drain(x_far), forward_gate(0)))
    hook(x_far + 4, lambda: forward_up(0))
    stages = [1 << b for b in reversed(range(n.bit_length() - 1))]
    hook(len(seq) // 2, functools.partial(mixed_stage, stages[0]))

    def to_side(p, d):
        theirs = lax.rem(sibling + 2 * d, q)
        return remote(
            part.at[rows(p), at_cols(theirs)],
            rsib.at[d, rows(p)],
            s2.at[p, d],
            r2.at[p, d],
            (s, sibling),
        )

    def to_far(p, d):
        return remote(
            pair.at[d - 1, rows(p)],
            ryb.at[d - 1, rows(p)],
            s3.at[p, d - 1],
            r3.at[p, d - 1],
            (s, lax.rem(t + 2 * d, q)),
        )

    def back(p):
        return remote(fin.at[rows(p)], ret.at[rows(p)], s4.at[p], r4.at[p], (peer(p), t))

    def mine(p, d):
        value = part[rows(p), at_cols(lax.rem(t + 2 * d, q))].astype(F32)
        return value + rsib[d, rows(p), :].astype(F32)

    def side_start(p):
        for d in [*range(1, ny), 0]:
            to_side(p, d).start()

    def pair_up(p):
        for d in range(1, ny):
            to_side(p, d).wait_recv()
            pair[d - 1, rows(p), :] = mine(p, d).astype(HALF)
            to_far(p, d).start()

    def finish(p):
        to_side(p, 0).wait_recv()
        value = mine(p, 0)
        for d in range(1, ny):
            to_far(p, d).wait_recv()
            value = value + ryb[d - 1, rows(p), :].astype(F32)
        if p:
            fin[rows(p), :] = value.astype(HALF)
            back(p).start()
        else:
            ret[rows(p), :] = value.astype(HALF)

    def own_batch():
        partial(own_rows)
        for k in reversed(own_ks):
            side_start(k)

    def own_pairs():
        for k in reversed(own_ks):
            pair_up(k)

    def far_half(h):
        drain(at[1, far_ks[len(far_ks) // 2 - 1 if h == 0 else -1]])
        back_hidden(far_halves[h])
        activation(far_halves[h])

    hook(x_own + 6, own_batch)
    hook(len(seq) - 2, own_pairs, lambda: far_half(0))
    hook(len(seq) - 1, lambda: far_half(1))

    for k, (a, p) in enumerate(seq):
        if k in ahead:
            ahead[k]()
        if p % top:
            first(a, p).wait_recv()
        for d in range(1, ny):
            across(a, p, d).start()
        beside(a, p, 0).start()
        if k >= lag:
            forward(k - lag)
        for call in hooks.get(k, []):
            call()

    forward(len(seq) - 1)
    partial(far_rows)
    for k in far_ks:
        side_start(k)
    mixed_stage(stages[1])
    drain(len(seq) - 1)
    back_hidden(rest_rows)
    for k in far_ks:
        pair_up(k)
    activation(rest_rows)
    for k in reversed(own_ks):
        finish(k)
    partial(rest_rows)
    for k in rest_ks:
        side_start(k)
    finish(far_ks[0])
    for k in rest_ks:
        pair_up(k)

    def weight_grad(left, a, target):
        def turn():
            turned[...] = left[...].astype(F32).T.astype(HALF)

        def piece(j):
            here = slice(j * cols, (j + 1) * cols)
            target[:, here] = lax.dot_general(
                turned[...], buf[a, :, here], PLAIN, preferred_element_type=F32
            ).astype(HALF)

        return [turn] + [functools.partial(piece, j) for j in range(q)]

    def some(work, count):
        for _ in range(min(count, len(work))):
            work.pop(0)()

    work = weight_grad(hid, 1, gdown_ref)
    for i, k in enumerate(far_ks[1:] + rest_ks):
        some(work, 1)
        finish(k)
        if 2 + i < len(stages):
            mixed_stage(stages[2 + i])
    some(work, len(work))
    for p in range(1, n):
        back(p).wait_recv()
    moe = jnp.dot(p_t[...], ret[...], preferred_element_type=F32)
    full_h[:, at_cols(t)] = (g_ref[...].astype(F32) + moe).astype(HALF)

    def h_across(d):
        b = full_h.at[:, at_cols(t)]
        return remote(b, b, shy.at[d - 1], rhy.at[d - 1], (s, lax.rem(t + 2 * d, q)))

    def h_beside(d):
        b = full_h.at[:, at_cols(lax.rem(t - 2 * d + q, q))]
        return remote(b, b, shs.at[d], rhs.at[d], (s, sibling))

    for d in range(1, ny):
        h_across(d).start()
    h_beside(0).start()

    def turn_h(tt):
        h_t[at_cols(tt), :] = full_h[:, at_cols(tt)].astype(F32).T.astype(HALF)

    turn_h(t)
    weights(3)
    work = weight_grad(dg, 0, ggate_ref)
    some(work, len(work))
    h_beside(0).wait_recv()
    turn_h(sibling)
    for d in range(1, ny):
        h_across(d).wait_recv()
        h_beside(d).start()
        turn_h(lax.rem(t - 2 * d + q, q))
    for d in range(1, ny):
        h_beside(d).wait_recv()
        turn_h(lax.rem(sibling - 2 * d + q, q))

    part_share = share // 2

    def half_rows(first_row):
        return pl.ds(
            pl.multiple_of(first_row + core * part_share, part_share), part_share
        )

    def h_far(p):
        return remote(
            h_t.at[half_rows(peer(p) * share)],
            all_t.at[half_rows(0), tokens(p)],
            sa.at[p],
            ra.at[p],
            (peer(p), t),
        )

    def h_pass(p):
        b = all_t.at[half_rows(0), tokens(p)]
        return remote(b, b, sf.at[p], rf.at[p], (s, sibling))

    send_order = [*far_ks, *rest_ks, *own_ks[1:]]
    for p in send_order:
        h_far(p).start()
    all_t[:, tokens(0)] = h_t[pl.ds(pl.multiple_of(s * share, share), share), :]

    def halo(k):
        there = lax.rem(s + 1, n) if k == 0 else lax.rem(s - 1 + n, n)
        return remote(edge.at[k], got.at[k], se.at[k], re.at[k], (there, t))

    grad_z = jnp.dot(full_h[...], wo[...], preferred_element_type=F32)
    dconv = (grad_z * b_ref[...].astype(F32)).astype(HALF).astype(F32)
    edge[0] = jnp.broadcast_to(dconv[tok - 1 : tok, :], (8, cols))
    edge[1] = jnp.broadcast_to(dconv[0:1, :], (8, cols))
    halo(0).start()
    halo(1).start()
    gb_ref[...] = (grad_z * co_ref[...].astype(F32)).astype(HALF)
    padded[8 : 8 + tok, :] = dconv
    work = weight_grad(du, 0, gup_ref)
    some(work, 3)
    for p in send_order:
        some(work, 1)
        h_far(p).wait_recv()
        h_pass(p).start()
    some(work, len(work))
    halo(0).wait_recv()
    halo(1).wait_recv()
    padded[0:8, :] = jnp.where(s > 0, got[0], 0.0)
    padded[8 + tok : 16 + tok, :] = jnp.where(s < n - 1, got[1], 0.0)
    grad_u = (
        taps_ref[0:1, :] * padded[9 : 9 + tok, :]
        + taps_ref[1:2, :] * padded[8 : 8 + tok, :]
        + taps_ref[2:3, :] * padded[7 : 7 + tok, :]
    )
    gc_ref[...] = (grad_u * v_ref[...].astype(F32)).astype(HALF)
    gv_ref[...] = (grad_u * c_ref[...].astype(F32)).astype(HALF)
    for k in range(1, n, 2):
        mixed(k).wait_recv()
    for p in send_order:
        h_pass(p).wait_recv()
    gout_ref[...] = jnp.dot(all_t[...], all_m[...], preferred_element_type=F32)

    for p in range(n):
        for a in range(2):
            if p % top:
                first(a, p).wait_send()
            for d in range(1, ny):
                across(a, p, d).wait_send()
            for d in range(ny):
                beside(a, p, d).wait_send()
        for d in range(ny):
            to_side(p, d).wait_send()
            if d:
                to_far(p, d).wait_send()
        if p:
            back(p).wait_send()
            h_far(p).wait_send()
            h_pass(p).wait_send()
            mixed(p).wait_send()
    for d in range(ny):
        if d:
            h_across(d).wait_send()
        h_beside(d).wait_send()
    for i in range(4):
        tokens_out(i).wait_send()
    halo(0).wait_send()
    halo(1).wait_send()


def layer(n, q, ids_t, weight_t, x, g, b, co, c, v, taps, wg, wu, wd, wo):
    tok, cols = x.shape
    units, width = wg.shape
    total = 4 * tok
    share = width // n
    ny = q // 2
    far = max(ny - 1, 1)
    vmem = pl.BlockSpec(memory_space=pltpu.VMEM)
    hbm = pl.BlockSpec(memory_space=pltpu.HBM)
    dma = pltpu.SemaphoreType.DMA
    like = pltpu.VMEM(g.shape, HALF)
    tall = pltpu.VMEM((units, width), HALF)

    def half(*shape):
        return pltpu.VMEM(shape, HALF)

    def full(*shape):
        return pltpu.VMEM(shape, F32)

    sems = [
        (2, n), (2, n, far), (2, n, ny), (n, ny), (n, far), (n,),
        (n,), (far,), (ny,), (n,), (n,), (2,),
    ]
    return pl.pallas_call(
        functools.partial(layer_kernel, n, q),
        out_shape=(
            pltpu.VMEM((share, cols), F32), like, like, like, tall, tall, tall,
        ),
        in_specs=[hbm] * 13,
        out_specs=(vmem,) * 7,
        scratch_shapes=[
            pltpu.VMEM(ids_t.shape, ids_t.dtype),
            full(*weight_t.shape),
            half(tok, cols),
            half(tok, cols),
            half(tok, cols),
            half(tok, cols),
            half(tok, cols),
            half(tok, cols),
            full(*taps.shape),
            half(units, width),
            half(units, width),
            half(units, width),
            half(width, cols),
            pltpu.VMEM(ids_t.shape, ids_t.dtype),
            full(*weight_t.shape),
            half(tok, cols),
            half(tok, cols),
            half(total // 2, 2 * tok),
            half(total // 2, tok),
            half(total, tok),
            half(tok, total),
            half(2, total // 2, cols),
            half(2, total // 2, cols),
            half(2, total, width),
            full(total, units),
            full(total, units),
            full(total, units),
            half(total, units),
            half(total, units),
            half(total, units),
            half(units, total),
            half(total, width),
            half(ny, total, cols),
            half(far, total, cols),
            half(far, total, cols),
            half(total, cols),
            half(total, cols),
            half(tok, width),
            half(width, tok),
            half(share, n * tok),
            half(n * tok, cols),
            full(2, 8, cols),
            full(2, 8, cols),
            full(tok + 16, cols),
            dma((13,)),
            dma((4,)),
            dma((4,)),
        ]
        + [dma(shape) for shape in sems for _ in range(2)],
        compiler_params=pltpu.CompilerParams(
            collective_id=0, has_side_effects=True, vmem_limit_bytes=44 * 2**20
        ),
        name="layer",
    )(
        *(
            pltpu.with_memory_space_constraint(a, pltpu.HBM)
            for a in (ids_t, weight_t, x, g, b, co, c, v, taps, wg, wu, wd, wo)
        )
    )


def settle_kernel(*refs):
    count = (len(refs) - 1) // 2
    sem = refs[-1]
    copies = [
        pltpu.make_async_copy(refs[k], refs[count + k], sem.at[k]) for k in range(count)
    ]
    for copy in copies:
        copy.start()
    for copy in copies:
        copy.wait()


def settle(*arrays):
    return pl.pallas_call(
        settle_kernel,
        out_shape=tuple(pltpu.HBM(a.shape, a.dtype) for a in arrays),
        in_specs=[pl.BlockSpec(memory_space=pltpu.VMEM)] * len(arrays),
        out_specs=(pl.BlockSpec(memory_space=pltpu.HBM),) * len(arrays),
        scratch_shapes=[pltpu.SemaphoreType.DMA((len(arrays),))],
        compiler_params=pltpu.CompilerParams(vmem_limit_bytes=2**20),
        name="settle",
    )(*(pltpu.with_memory_space_constraint(a, pltpu.VMEM) for a in arrays))


def local(
    out_grad,
    moe_input,
    route_weight,
    route_ids,
    gate_proj,
    up_proj,
    down_proj,
    out_proj,
    conv_out,
    gate_b,
    gate_c,
    value_v,
    conv_taps,
):
    n = lax.axis_size("sp")
    q = lax.axis_size("tp")
    results = layer(
        n, q, route_ids.T, route_weight.T, moe_input, out_grad, gate_b, conv_out, gate_c,
        value_v, conv_taps, gate_proj[0].T, up_proj[0].T, down_proj[0], out_proj,
    )
    grad_out, grad_b, grad_c, grad_v, grad_gate, grad_up, grad_down = settle(*results)
    return (grad_gate.T[None], grad_up.T[None], grad_down[None], grad_out, grad_b, grad_c, grad_v)


def solution(mesh):
    in_specs = (
        P("sp", "tp"),
        P("sp", "tp"),
        P("sp", None),
        P("sp", None),
        P("sp", None, "tp"),
        P("sp", None, "tp"),
        P("sp", "tp", None),
        P(None, "tp"),
        P("sp", "tp"),
        P("sp", "tp"),
        P("sp", "tp"),
        P("sp", "tp"),
        P(None, "tp"),
    )
    out_specs = (
        P("sp", None, "tp"),
        P("sp", None, "tp"),
        P("sp", "tp", None),
        P("sp", "tp"),
        P("sp", "tp"),
        P("sp", "tp"),
        P("sp", "tp"),
    )
    return jax.shard_map(local, mesh=mesh, in_specs=in_specs, out_specs=out_specs, check_vma=False)
```

```python
import functools

import jax
import jax.numpy as jnp
from jax import lax
from jax.experimental import pallas as pl
from jax.experimental.pallas import tpu as pltpu
from jax.sharding import PartitionSpec as P

MESH = pl.DeviceIdType.MESH
HALF = jnp.bfloat16
F32 = jnp.float32
PLAIN = (((1,), (0,)), ((), ()))
RIGHT_T = (((1,), (1,)), ((), ()))


def remote(src, dst, send_sem, recv_sem, device):
    return pltpu.make_async_remote_copy(
        src_ref=src,
        dst_ref=dst,
        send_sem=send_sem,
        recv_sem=recv_sem,
        device_id=device,
        device_id_type=MESH,
    )


def layer_kernel(
    n, q,
    ids_hbm, rw_hbm, x_hbm, g_hbm, b_hbm, co_hbm, c_hbm, v_hbm, taps_hbm,
    wg_hbm, wu_hbm, wd_hbm, wo_hbm,
    gout_ref, gb_ref, gc_ref, gv_ref, ggate_ref, gup_ref, gdown_ref,
    ids_ref, rw_ref, x_ref, g_ref, b_ref, co_ref, c_ref, v_ref, taps_ref,
    wg, wu, wd, wo, ids_in, rw_in, x_in, g_in, p01, p_in, p_ref, p_t, send, send_in, buf, gate, upval, dhid, hid, dg, du, turned,
    part, rsib, pair, ryb, fin, ret, full_h, h_t, all_t, all_m, edge, got, padded,
    w_sem, st, rt,
    s1, r1, sy, ry, ss, rs, s2, r2, s3, r3, s4, r4,
    sm, rm, shy, rhy, shs, rhs, sa, ra, sf, rf, se, re,
):
    s, t = lax.axis_index("sp"), lax.axis_index("tp")
    core = lax.rem(t, 2)
    sibling = t + 1 - 2 * core
    ny = q // 2
    tok, cols = x_ref.shape
    total, width = part.shape
    cap = total // n
    share = width // n
    units = wg.shape[0]
    top = n // 2
    batch = total // 2

    barrier = pltpu.get_barrier_semaphore()
    for i in range(1, n):
        pl.semaphore_signal(
            barrier, inc=1, device_id=(lax.rem(s + i, n), t), device_id_type=MESH
        )
    for d in range(1, ny):
        pl.semaphore_signal(
            barrier, inc=1, device_id=(s, lax.rem(t + 2 * d, q)), device_id_type=MESH
        )
    pl.semaphore_signal(barrier, inc=1, device_id=(s, sibling), device_id_type=MESH)

    loads = [
        pltpu.make_async_copy(source, target, w_sem.at[k])
        for k, (source, target) in enumerate(
            zip(
                (
                    wg_hbm, wu_hbm, wd_hbm, wo_hbm, ids_hbm, x_hbm, rw_hbm, g_hbm,
                    b_hbm, co_hbm, c_hbm, v_hbm, taps_hbm,
                ),
                (
                    wg, wu, wd, wo, ids_ref, x_ref, rw_ref, g_ref,
                    b_ref, co_ref, c_ref, v_ref, taps_ref,
                ),
            )
        )
    ]
    for load in [*loads[4:], *loads[:4]]:
        load.start()

    def peer(k):
        value = s
        for b in range(n.bit_length() - 1):
            if k >> b & 1:
                value = value + (1 - 2 * lax.rem(lax.div(s, 1 << b), 2)) * (1 << b)
        return value

    def rows(k):
        p = k ^ top
        return slice(p * cap, (p + 1) * cap)

    def near_rows(k):
        return slice(k * cap, (k + 1) * cap)

    def at_cols(tt):
        return pl.ds(pl.multiple_of(tt * cols, cols), cols)

    row_i = lax.broadcasted_iota(jnp.int32, (tok, tok), 0)
    col_i = lax.broadcasted_iota(jnp.int32, (tok, tok), 1)
    slots = lax.broadcasted_iota(jnp.int32, (cap, tok), 0)

    def choices(ids, ks):
        ids0, ids1 = ids[0:1, :], ids[1:2, :]
        where = lax.broadcasted_iota(jnp.int32, (n, tok), 0)
        experts = jnp.full((n, tok), -1, jnp.int32)
        for i, k in enumerate(ks):
            experts = jnp.where(where == i, peer(k), experts)
        named = jnp.logical_or(ids0 == experts, ids1 == experts)
        before = jnp.dot(
            jnp.where(named, 1.0, 0.0).astype(HALF),
            jnp.where(row_i < col_i, 1.0, 0.0).astype(HALF),
            preferred_element_type=F32,
        ).astype(jnp.int32)
        for i, k in enumerate(ks):
            here = before[i : i + 1, :] == slots
            c0 = jnp.where(jnp.logical_and(here, ids0 == peer(k)), 1.0, 0.0)
            c1 = jnp.where(jnp.logical_and(here, ids1 == peer(k)), 1.0, 0.0)
            yield k, c0, c1

    def weighted(rw, g):
        grad = g[...].astype(F32)
        parts = []
        for k in range(2):
            column = jnp.sum(
                jnp.where(row_i == col_i, rw[k : k + 1, :], 0.0), axis=1, keepdims=True
            )
            parts.append((column * grad).astype(HALF))
        return jnp.concatenate(parts, axis=0)

    def tokens_out(i):
        here, there = ((ids_ref, ids_in), (x_ref, x_in), (rw_ref, rw_in), (g_ref, g_in))[i]
        return remote(here, there, st.at[i], rt.at[i], (peer(top), t))

    def first(a, k):
        if k < top:
            rows_out = send.at[a, near_rows(k)]
        else:
            rows_out = send_in.at[a, near_rows(k ^ top)]
        return remote(
            rows_out,
            buf.at[a, rows(k), at_cols(t)],
            s1.at[a, k],
            r1.at[a, k],
            (peer(k % top), t),
        )

    def across(a, p, d):
        b = buf.at[a, rows(p), at_cols(t)]
        return remote(
            b, b, sy.at[a, p, d - 1], ry.at[a, p, d - 1], (s, lax.rem(t + 2 * d, q))
        )

    def beside(a, p, d):
        b = buf.at[a, rows(p), at_cols(lax.rem(t - 2 * d + q, q))]
        return remote(b, b, ss.at[a, p, d], rs.at[a, p, d], (s, sibling))

    near = [*range(1, top)]
    own_ks, rest_ks = [*range(top // 2)], [*range(top // 2, top)]
    far_ks = [*range(top, n)]

    loads[4].wait()
    loads[5].wait()
    pl.semaphore_wait(barrier, n - 1 + ny)
    tokens_out(0).start()
    tokens_out(1).start()
    for k, c0, c1 in choices(ids_ref, range(top)):
        p01[near_rows(k), 0:tok] = c0.astype(HALF)
        p01[near_rows(k), tok : 2 * tok] = c1.astype(HALF)
        p_ref[rows(k), :] = (c0 + c1).astype(HALF)
    send[0] = jnp.dot(
        p_ref[batch:total, :], x_ref[...], preferred_element_type=F32
    ).astype(HALF)
    for k in near:
        first(0, k).start()
    buf[0, rows(0), at_cols(t)] = send[0, near_rows(0), :]
    loads[6].wait()
    loads[7].wait()
    tokens_out(2).start()
    tokens_out(3).start()
    send[1] = jnp.dot(
        p01[...], weighted(rw_ref, g_ref), preferred_element_type=F32
    ).astype(HALF)
    for k in own_ks[1:]:
        first(1, k).start()
    buf[1, rows(0), at_cols(t)] = send[1, near_rows(0), :]

    def sort_x():
        tokens_out(0).wait_recv()
        tokens_out(1).wait_recv()
        for k, c0, c1 in choices(ids_in, range(top)):
            p01[near_rows(k), 0:tok] = c0.astype(HALF)
            p01[near_rows(k), tok : 2 * tok] = c1.astype(HALF)
            p_in[near_rows(k), :] = (c0 + c1).astype(HALF)
        send_in[0] = jnp.dot(
            p_in[...], x_in[...], preferred_element_type=F32
        ).astype(HALF)
        for k in near:
            first(0, k ^ top).start()
        buf[0, rows(top), at_cols(t)] = send_in[0, near_rows(0), :]

    def sort_g():
        tokens_out(2).wait_recv()
        tokens_out(3).wait_recv()
        send_in[1] = jnp.dot(
            p01[...], weighted(rw_in, g_in), preferred_element_type=F32
        ).astype(HALF)
        for k in near:
            first(1, k ^ top).start()
        for k in rest_ks:
            first(1, k).start()
        buf[1, rows(top), at_cols(t)] = send_in[1, near_rows(0), :]

    def forward_units(at):
        for values, w in ((gate, wg), (upval, wu)):
            values[at, :] = lax.dot_general(
                buf[0, at, :], w[...], RIGHT_T, preferred_element_type=F32
            )

    def back_hidden(at):
        dhid[at, :] = lax.dot_general(
            buf[1, at, :], wd[...], RIGHT_T, preferred_element_type=F32
        )

    step_rows = 32

    def activation(span_at):
        def step(r, _):
            at = pl.ds(
                pl.multiple_of(span_at.start + r * step_rows, step_rows), step_rows
            )
            z, u, dh = gate[at, :], upval[at, :], dhid[at, :]
            sig = jax.nn.sigmoid(z)
            act = z * sig
            hid[at, :] = (act * u).astype(HALF)
            dg[at, :] = (dh * u * (sig * (1.0 + z * (1.0 - sig)))).astype(HALF)
            du[at, :] = (dh * act).astype(HALF)
            return 0

        lax.fori_loop(0, (span_at.stop - span_at.start) // step_rows, step, 0)

    def partial(at, tt):
        here = at_cols(tt)
        part[at, here] = (
            lax.dot_general(dg[at, :], wg[:, here], PLAIN, preferred_element_type=F32)
            + lax.dot_general(du[at, :], wu[:, here], PLAIN, preferred_element_type=F32)
        ).astype(HALF)

    far_rows, more_rows, own_rows, rest_rows = (
        slice(i * batch // 2, (i + 1) * batch // 2) for i in range(4)
    )
    more_ks = far_ks[len(far_ks) // 2 :]
    near_far_ks = far_ks[: len(far_ks) // 2]

    seq = [(a, k) for k in own_ks for a in range(2)]
    seq += [(0, k) for k in rest_ks + far_ks[:-1]] + [(1, far_ks[0]), (0, far_ks[-1])]
    seq += [(1, k) for k in far_ks[1:] + rest_ks]
    lag = 3
    forwarded, drained = set(), set()

    def forward(upto):
        for k in range(upto + 1):
            if k not in forwarded:
                forwarded.add(k)
                for d in range(1, ny):
                    across(*seq[k], d).wait_recv()
                    beside(*seq[k], d).start()

    def drain(upto):
        forward(upto)
        for k in range(upto + 1):
            if k not in drained:
                drained.add(k)
                for d in range(ny):
                    beside(*seq[k], d).wait_recv()

    def weights(k):
        loads[k].wait()

    def tokens(k):
        p = k ^ top
        return slice(p * tok, (p + 1) * tok)

    def mixed(k):
        low = k & -k
        return remote(
            all_m.at[tokens(k ^ low)], all_m.at[tokens(k)], sm.at[k], rm.at[k], (peer(low), t)
        )

    def mixed_own():
        for k in range(8, 13):
            loads[k].wait()
        all_m[tokens(0), :] = (b_ref[...].astype(F32) * co_ref[...].astype(F32)).astype(HALF)

    def mixed_stage(low):
        for k in range(0, n, 2 * low):
            if k & -k == 2 * low:
                mixed(k).wait_recv()
        for k in range(low, n, 2 * low):
            mixed(k).start()

    def turn_slots():
        for k, c0, c1 in choices(ids_ref, far_ks):
            p_ref[rows(k), :] = (c0 + c1).astype(HALF)
        p_t[...] = p_ref[...].astype(F32).T.astype(HALF)

    ahead, hooks = {}, {}

    def hook(k, *calls):
        hooks.setdefault(min(k, len(seq) - 1), []).extend(calls)

    at = {unit: k for k, unit in enumerate(seq)}
    x_own, x_far = at[0, top - 1], at[0, n - 1]
    ahead[at[0, rest_ks[-1]]] = sort_x
    ahead[at[0, more_ks[0]]] = lambda: (forward(x_own), sort_g())
    stages = [1 << b for b in reversed(range(n.bit_length() - 1))]
    hook(1, mixed_own)
    hook(3, turn_slots)
    hook(
        at[1, far_ks[0]],
        lambda: (drain(x_own), weights(0), weights(1), forward_units(slice(batch, total))),
    )
    hook(
        x_far,
        functools.partial(mixed_stage, stages[0]),
        lambda: (drain(at[1, own_ks[-1]]), weights(2), back_hidden(own_rows)),
        lambda: activation(own_rows),
    )

    def to_side(p, d):
        theirs = lax.rem(sibling + 2 * d, q)
        return remote(
            part.at[rows(p), at_cols(theirs)],
            rsib.at[d, rows(p)],
            s2.at[p, d],
            r2.at[p, d],
            (s, sibling),
        )

    def to_far(p, d):
        return remote(
            pair.at[d - 1, rows(p)],
            ryb.at[d - 1, rows(p)],
            s3.at[p, d - 1],
            r3.at[p, d - 1],
            (s, lax.rem(t + 2 * d, q)),
        )

    def back(p):
        return remote(fin.at[rows(p)], ret.at[rows(p)], s4.at[p], r4.at[p], (peer(p), t))

    def mine(p, d):
        value = part[rows(p), at_cols(lax.rem(t + 2 * d, q))].astype(F32)
        return value + rsib[d, rows(p), :].astype(F32)

    def input_grads(at, ks, pairs_too, done=()):
        for d in [*range(1, ny), 0]:
            partial(at, lax.rem(sibling + 2 * d, q))
            for k in ks:
                to_side(k, d).start()
            if pairs_too and d == 0:
                for k in ks:
                    pair_up(k)
                for k in done[len(done) // 2 :]:
                    finish(k)
            partial(at, lax.rem(t + 2 * d, q))
            if d == ny - 1:
                for k in done[: len(done) // 2]:
                    finish(k)

    def pair_up(p):
        for d in range(1, ny):
            to_side(p, d).wait_recv()
            pair[d - 1, rows(p), :] = mine(p, d).astype(HALF)
            to_far(p, d).start()

    def finish(p):
        to_side(p, 0).wait_recv()
        value = mine(p, 0)
        for d in range(1, ny):
            to_far(p, d).wait_recv()
            value = value + ryb[d - 1, rows(p), :].astype(F32)
        if p:
            fin[rows(p), :] = value.astype(HALF)
            back(p).start()
        else:
            ret[rows(p), :] = value.astype(HALF)

    def own_pairs():
        for k in reversed(own_ks):
            pair_up(k)

    hook(at[1, far_ks[2]], lambda: input_grads(own_rows, own_ks[::-1], False))
    hook(at[1, far_ks[-1]], own_pairs)
    hook(
        at[1, rest_ks[0]],
        lambda: (drain(x_far), forward_units(slice(0, batch))),
        lambda: (drain(at[1, near_far_ks[-1]]), back_hidden(far_rows)),
        lambda: activation(far_rows),
    )

    for k, (a, p) in enumerate(seq):
        if k in ahead:
            ahead[k]()
        if p % top:
            first(a, p).wait_recv()
        for d in range(1, ny):
            across(a, p, d).start()
        beside(a, p, 0).start()
        if k >= lag:
            forward(k - lag)
        for call in hooks.get(k, []):
            call()

    input_grads(far_rows, near_far_ks, True)
    mixed_stage(stages[1])
    drain(at[1, far_ks[-1]])
    back_hidden(more_rows)
    activation(more_rows)
    for k in reversed(own_ks):
        finish(k)
    input_grads(more_rows, more_ks, True, near_far_ks)
    drain(len(seq) - 1)
    back_hidden(rest_rows)
    activation(rest_rows)
    input_grads(rest_rows, rest_ks, True, more_ks)

    def weight_grad(left, a, target):
        def turn():
            turned[...] = left[...].astype(F32).T.astype(HALF)

        def piece(j):
            here = slice(j * cols, (j + 1) * cols)
            target[:, here] = lax.dot_general(
                turned[...], buf[a, :, here], PLAIN, preferred_element_type=F32
            ).astype(HALF)

        return [turn] + [functools.partial(piece, j) for j in range(q)]

    def some(work, count):
        for _ in range(min(count, len(work))):
            work.pop(0)()

    work = weight_grad(hid, 1, gdown_ref)
    some(work, 2)
    for low in stages[2:]:
        mixed_stage(low)
    for i, k in enumerate(rest_ks):
        some(work, 1)
        finish(k)
    some(work, len(work))
    for p in range(1, n):
        back(p).wait_recv()
    moe = jnp.dot(p_t[...], ret[...], preferred_element_type=F32)
    full_h[:, at_cols(t)] = (g_ref[...].astype(F32) + moe).astype(HALF)

    def h_across(d):
        b = full_h.at[:, at_cols(t)]
        return remote(b, b, shy.at[d - 1], rhy.at[d - 1], (s, lax.rem(t + 2 * d, q)))

    def h_beside(d):
        b = full_h.at[:, at_cols(lax.rem(t - 2 * d + q, q))]
        return remote(b, b, shs.at[d], rhs.at[d], (s, sibling))

    for d in range(1, ny):
        h_across(d).start()
    h_beside(0).start()

    def turn_h(tt):
        h_t[at_cols(tt), :] = full_h[:, at_cols(tt)].astype(F32).T.astype(HALF)

    turn_h(t)
    weights(3)
    work = weight_grad(dg, 0, ggate_ref)
    some(work, len(work))
    h_beside(0).wait_recv()
    turn_h(sibling)
    for d in range(1, ny):
        h_across(d).wait_recv()
        h_beside(d).start()
        turn_h(lax.rem(t - 2 * d + q, q))
    for d in range(1, ny):
        h_beside(d).wait_recv()
        turn_h(lax.rem(sibling - 2 * d + q, q))

    part_share = share // 2

    def half_rows(first_row):
        return pl.ds(
            pl.multiple_of(first_row + core * part_share, part_share), part_share
        )

    def h_far(p):
        return remote(
            h_t.at[half_rows(peer(p) * share)],
            all_t.at[half_rows(0), tokens(p)],
            sa.at[p],
            ra.at[p],
            (peer(p), t),
        )

    def h_pass(p):
        b = all_t.at[half_rows(0), tokens(p)]
        return remote(b, b, sf.at[p], rf.at[p], (s, sibling))

    send_order = [*far_ks, *rest_ks, *own_ks[1:]]
    for p in send_order:
        h_far(p).start()
    all_t[:, tokens(0)] = h_t[pl.ds(pl.multiple_of(s * share, share), share), :]

    def halo(k):
        there = lax.rem(s + 1, n) if k == 0 else lax.rem(s - 1 + n, n)
        return remote(edge.at[k], got.at[k], se.at[k], re.at[k], (there, t))

    grad_z = jnp.dot(full_h[...], wo[...], preferred_element_type=F32)
    dconv = (grad_z * b_ref[...].astype(F32)).astype(HALF).astype(F32)
    edge[0] = jnp.broadcast_to(dconv[tok - 1 : tok, :], (8, cols))
    edge[1] = jnp.broadcast_to(dconv[0:1, :], (8, cols))
    halo(0).start()
    halo(1).start()
    gb_ref[...] = (grad_z * co_ref[...].astype(F32)).astype(HALF)
    padded[8 : 8 + tok, :] = dconv
    work = weight_grad(du, 0, gup_ref)
    some(work, 3)
    for p in send_order:
        some(work, 1)
        h_far(p).wait_recv()
        h_pass(p).start()
    some(work, len(work))
    halo(0).wait_recv()
    halo(1).wait_recv()
    padded[0:8, :] = jnp.where(s > 0, got[0], 0.0)
    padded[8 + tok : 16 + tok, :] = jnp.where(s < n - 1, got[1], 0.0)
    grad_u = (
        taps_ref[0:1, :] * padded[9 : 9 + tok, :]
        + taps_ref[1:2, :] * padded[8 : 8 + tok, :]
        + taps_ref[2:3, :] * padded[7 : 7 + tok, :]
    )
    gc_ref[...] = (grad_u * v_ref[...].astype(F32)).astype(HALF)
    gv_ref[...] = (grad_u * c_ref[...].astype(F32)).astype(HALF)
    for k in range(1, n, 2):
        mixed(k).wait_recv()
    for p in send_order:
        h_pass(p).wait_recv()
    gout_ref[...] = jnp.dot(all_t[...], all_m[...], preferred_element_type=F32)

    for p in range(n):
        for a in range(2):
            if p % top:
                first(a, p).wait_send()
            for d in range(1, ny):
                across(a, p, d).wait_send()
            for d in range(ny):
                beside(a, p, d).wait_send()
        for d in range(ny):
            to_side(p, d).wait_send()
            if d:
                to_far(p, d).wait_send()
        if p:
            back(p).wait_send()
            h_far(p).wait_send()
            h_pass(p).wait_send()
            mixed(p).wait_send()
    for d in range(ny):
        if d:
            h_across(d).wait_send()
        h_beside(d).wait_send()
    for i in range(4):
        tokens_out(i).wait_send()
    halo(0).wait_send()
    halo(1).wait_send()


def layer(n, q, ids_t, weight_t, x, g, b, co, c, v, taps, wg, wu, wd, wo):
    tok, cols = x.shape
    units, width = wg.shape
    total = 4 * tok
    share = width // n
    ny = q // 2
    far = max(ny - 1, 1)
    vmem = pl.BlockSpec(memory_space=pltpu.VMEM)
    hbm = pl.BlockSpec(memory_space=pltpu.HBM)
    dma = pltpu.SemaphoreType.DMA
    like = pltpu.VMEM(g.shape, HALF)
    tall = pltpu.VMEM((units, width), HALF)

    def half(*shape):
        return pltpu.VMEM(shape, HALF)

    def full(*shape):
        return pltpu.VMEM(shape, F32)

    sems = [
        (2, n), (2, n, far), (2, n, ny), (n, ny), (n, far), (n,),
        (n,), (far,), (ny,), (n,), (n,), (2,),
    ]
    return pl.pallas_call(
        functools.partial(layer_kernel, n, q),
        out_shape=(
            pltpu.VMEM((share, cols), F32), like, like, like, tall, tall, tall,
        ),
        in_specs=[hbm] * 13,
        out_specs=(vmem,) * 7,
        scratch_shapes=[
            pltpu.VMEM(ids_t.shape, ids_t.dtype),
            full(*weight_t.shape),
            half(tok, cols),
            half(tok, cols),
            half(tok, cols),
            half(tok, cols),
            half(tok, cols),
            half(tok, cols),
            full(*taps.shape),
            half(units, width),
            half(units, width),
            half(units, width),
            half(width, cols),
            pltpu.VMEM(ids_t.shape, ids_t.dtype),
            full(*weight_t.shape),
            half(tok, cols),
            half(tok, cols),
            half(total // 2, 2 * tok),
            half(total // 2, tok),
            half(total, tok),
            half(tok, total),
            half(2, total // 2, cols),
            half(2, total // 2, cols),
            half(2, total, width),
            full(total, units),
            full(total, units),
            full(total, units),
            half(total, units),
            half(total, units),
            half(total, units),
            half(units, total),
            half(total, width),
            half(ny, total, cols),
            half(far, total, cols),
            half(far, total, cols),
            half(total, cols),
            half(total, cols),
            half(tok, width),
            half(width, tok),
            half(share, n * tok),
            half(n * tok, cols),
            full(2, 8, cols),
            full(2, 8, cols),
            full(tok + 16, cols),
            dma((13,)),
            dma((4,)),
            dma((4,)),
        ]
        + [dma(shape) for shape in sems for _ in range(2)],
        compiler_params=pltpu.CompilerParams(
            collective_id=0, has_side_effects=True, vmem_limit_bytes=44 * 2**20
        ),
        name="layer",
    )(
        *(
            pltpu.with_memory_space_constraint(a, pltpu.HBM)
            for a in (ids_t, weight_t, x, g, b, co, c, v, taps, wg, wu, wd, wo)
        )
    )


def settle_kernel(*refs):
    count = (len(refs) - 1) // 2
    sem = refs[-1]
    copies = [
        pltpu.make_async_copy(refs[k], refs[count + k], sem.at[k]) for k in range(count)
    ]
    for copy in copies:
        copy.start()
    for copy in copies:
        copy.wait()


def settle(*arrays):
    return pl.pallas_call(
        settle_kernel,
        out_shape=tuple(pltpu.HBM(a.shape, a.dtype) for a in arrays),
        in_specs=[pl.BlockSpec(memory_space=pltpu.VMEM)] * len(arrays),
        out_specs=(pl.BlockSpec(memory_space=pltpu.HBM),) * len(arrays),
        scratch_shapes=[pltpu.SemaphoreType.DMA((len(arrays),))],
        compiler_params=pltpu.CompilerParams(vmem_limit_bytes=2**20),
        name="settle",
    )(*(pltpu.with_memory_space_constraint(a, pltpu.VMEM) for a in arrays))


def local(
    out_grad,
    moe_input,
    route_weight,
    route_ids,
    gate_proj,
    up_proj,
    down_proj,
    out_proj,
    conv_out,
    gate_b,
    gate_c,
    value_v,
    conv_taps,
):
    n = lax.axis_size("sp")
    q = lax.axis_size("tp")
    results = layer(
        n, q, route_ids.T, route_weight.T, moe_input, out_grad, gate_b, conv_out, gate_c,
        value_v, conv_taps, gate_proj[0].T, up_proj[0].T, down_proj[0], out_proj,
    )
    grad_out, grad_b, grad_c, grad_v, grad_gate, grad_up, grad_down = settle(*results)
    return (grad_gate.T[None], grad_up.T[None], grad_down[None], grad_out, grad_b, grad_c, grad_v)


def solution(mesh):
    in_specs = (
        P("sp", "tp"),
        P("sp", "tp"),
        P("sp", None),
        P("sp", None),
        P("sp", None, "tp"),
        P("sp", None, "tp"),
        P("sp", "tp", None),
        P(None, "tp"),
        P("sp", "tp"),
        P("sp", "tp"),
        P("sp", "tp"),
        P("sp", "tp"),
        P(None, "tp"),
    )
    out_specs = (
        P("sp", None, "tp"),
        P("sp", None, "tp"),
        P("sp", "tp", None),
        P("sp", "tp"),
        P("sp", "tp"),
        P("sp", "tp"),
        P("sp", "tp"),
    )
    return jax.shard_map(local, mesh=mesh, in_specs=in_specs, out_specs=out_specs, check_vma=False)
```
